512 devices in a mesh: sp: 16 (over z), dp: 32 (over y, x, core).
Axes of the slice: x: 4, y: 4, z: 16, core: 2. Of those that a mesh axis runs over, the one named last changes fastest.
Arguments:
- queries: bfloat16 [32, 3072, 16, 128], P('dp', 'sp'), may hold values from -6 to 6
- keys: bfloat16 [32, 3072, 16, 128], P('dp', 'sp'), may hold values from -6 to 6
- values: bfloat16 [32, 3072, 16, 128], P('dp', 'sp'), may hold values from -6 to 6
- mix_ratio: float32 [16], replicated, may hold values from 0.3 to 0.8
- out_gain: float32 [128], replicated, may hold values from 0.1 to 1.9
- out_weight: bfloat16 [2048, 2048], P(None, 'dp'), may hold values from -0.125 to 0.125
Outputs:
- layer_out: bfloat16 [32, 3072, 2048], P('dp', 'sp')
The draws below stay inside these ranges and needn't reach their ends.
All inputs are finite; a program needn't handle non-finite values.
Results may differ from the reference program's by a relative error of at most 0.0098.
Values may be sent and summed in bfloat16 or wider, within the bound.
A program may use at most 64 MiB of HBM per device.

```python
import math
import jax
import jax.numpy as jnp
from jax import lax

D = 2048
HEADS = 16
KEY_DIM = 64
HEAD_DIM = 128
SEQS = 32
LENGTH = 3072


def score_field(key, salt):
    shape = (SEQS, LENGTH, HEADS, 2 * KEY_DIM)
    spread = jnp.clip(1.3 * jax.random.normal(jax.random.fold_in(key, salt), shape, jnp.float32), -6.0, 6.0)
    return spread.astype(jnp.bfloat16)


def draw_queries(key, part):
    return score_field(key, 1)


def draw_keys(key, part):
    return score_field(key, 2)


def block_levels(stream_key, dims, shards, smallest, high):
    level, own = 1.0, jax.random.fold_in(stream_key, 6)
    for dim, blocks in shards:
        heights = jnp.exp(jax.random.uniform(jax.random.fold_in(own, dim), (blocks,), jnp.float32, smallest / len(shards), high / len(shards)))
        level = level * jnp.repeat(heights, dims[dim] // blocks).reshape([-1 if axis == dim else 1 for axis in range(len(dims))])
    return level


def bell_draw(rng, shape, scale, bound, pieces=(), kind=jnp.bfloat16):
    loudness = block_levels(rng, shape, pieces, -0.22, 0.18) if pieces else 1.0
    array = jax.random.normal(rng, shape, jnp.float32) * scale * loudness
    return jnp.minimum(jnp.maximum(array, -bound), bound).astype(kind)


def setup_inputs(seed: int = 0) -> dict:
    streams_of = jax.random.split(jax.random.key(seed), 7)
    return {
        "queries": draw_queries(jax.random.fold_in(streams_of[6], 71), 0),
        "keys": draw_keys(jax.random.fold_in(streams_of[6], 71), 0),
        "values": bell_draw(streams_of[2], (SEQS, LENGTH, HEADS, HEAD_DIM), 1.0, 6.0, ((0, 32), (1, 16))),
        "mix_ratio": jnp.clip(jax.random.uniform(streams_of[3], (HEADS,), jnp.float32, 0.3, 0.8), 0.3, 0.8),
        "out_gain": jnp.clip(1.0 + 0.18 * jax.random.normal(streams_of[4], (HEAD_DIM,), jnp.float32), 0.1, 1.9),
        "out_weight": bell_draw(streams_of[5], (HEADS * HEAD_DIM, D), (HEADS * HEAD_DIM) ** -0.5, 0.125, ((1, 32),)),
    }


theta_base = 500000.0
neg_large = -1e+30
norm_eps = 1e-05

def rotate_halves(field, positions):
    width = field.shape[-1] // 2
    half = width // 2
    freqs = theta_base ** (-jnp.arange(half, dtype=jnp.float32) * 2.0 / width)
    angle = positions.astype(jnp.float32)[:, None] * freqs[None, :]
    cosine = jnp.cos(angle)[:, None, :]
    sine = jnp.sin(angle)[:, None, :]
    parts = field.reshape(field.shape[0], 2, width)
    lower = parts[..., :half]
    upper = parts[..., half:]
    turned = jnp.concatenate([lower * cosine - upper * sine, upper * cosine + lower * sine], axis=-1)
    return turned.reshape(field.shape)

def masked_softmax(scores, visible):
    kept = jnp.where(visible, scores, neg_large)
    highest = lax.optimization_barrier(jnp.max(kept, axis=-1, keepdims=True))
    powers = jnp.exp(kept - highest)
    return powers / lax.optimization_barrier(jnp.sum(powers, axis=-1, keepdims=True))

def head_attention(query_head, key_head, value_head, ratio, gain):
    length = query_head.shape[0]
    width = query_head.shape[1] // 2
    positions = jnp.arange(length, dtype=jnp.int32)
    rotated_queries = (rotate_halves(query_head.astype(jnp.float32), positions) * width ** (-0.5)).astype(jnp.bfloat16)
    rotated_keys = rotate_halves(key_head.astype(jnp.float32), positions).astype(jnp.bfloat16)
    block = math.gcd(512, length)

    def one_block(start):
        query_rows = lax.dynamic_slice_in_dim(rotated_queries, start, block, 0)
        visible = (start + jnp.arange(block, dtype=jnp.int32))[:, None] >= positions[None, :]
        first = jnp.dot(query_rows[:, :width], rotated_keys[:, :width].T, preferred_element_type=jnp.float32)
        second = jnp.dot(query_rows[:, width:], rotated_keys[:, width:].T, preferred_element_type=jnp.float32)
        weights = (masked_softmax(first, visible) - ratio * masked_softmax(second, visible)).astype(jnp.bfloat16)
        mixed = jnp.dot(weights, value_head, preferred_element_type=jnp.float32)
        scale = lax.rsqrt(lax.optimization_barrier(jnp.mean(mixed * mixed, axis=-1, keepdims=True)) + norm_eps)
        return (mixed * scale * gain).astype(jnp.bfloat16)
    starts = jnp.arange(length // block, dtype=jnp.int32) * block
    return lax.map(one_block, starts).reshape(length, value_head.shape[1])

def reference(queries, keys, values, mix_ratio, out_gain, out_weight):

    def one_sequence(items):
        query_seq, key_seq, value_seq = items

        def one_head(head_items):
            query_head, key_head, value_head, ratio = head_items
            return head_attention(query_head, key_head, value_head, ratio, out_gain)
        heads = lax.map(one_head, (jnp.swapaxes(query_seq, 0, 1), jnp.swapaxes(key_seq, 0, 1), jnp.swapaxes(value_seq, 0, 1), mix_ratio))
        attended = jnp.swapaxes(heads, 0, 1).reshape(query_seq.shape[0], -1)
        return jnp.dot(attended, out_weight, preferred_element_type=jnp.float32).astype(jnp.bfloat16)
    return lax.map(one_sequence, (queries, keys, values))
```

```python
import functools

import jax
import jax.numpy as jnp
import numpy as np
from jax import lax
from jax.experimental import pallas as pl
from jax.experimental.pallas import tpu as pltpu
from jax.sharding import PartitionSpec as P

theta_base = 500000.0
neg_large = -1e30
norm_eps = 1e-05
MESH = pl.DeviceIdType.MESH
f32, bf16 = jnp.float32, jnp.bfloat16
CHUNK = 384


def peer_order(n):
    order = []
    for d in range(1, n // 2 + 1):
        order.append(d)
        if n - d != d:
            order.append(n - d)
    return order


def dot_nt(a, b):
    return lax.dot_general(a, b, (((1,), (1,)), ((), ())), preferred_element_type=f32)


def kernel(
    n, cores, rows, cols,
    mix_ref, q_hbm, k_hbm, v_hbm, gain_ref, freq_ref, w_hbm, out_ref,
    xin, win, xf, cos_s, sin_s, vs, ks, qs, vr, kr, qr, ob, ar, wt, qst, sc, mx, acc, oacc,
    in_sem, vss, kss, qss, oss, wss, wfs, vrs, krs, qrs, ars, wrs, wfr,
):
    me = lax.axis_index("sp")
    dp = lax.axis_index("dp")
    core = lax.rem(dp, 2)
    chip = lax.div(dp, 2)
    chips = cores // 2
    order = peer_order(n)

    loads = []
    for t, src in enumerate((v_hbm, k_hbm, q_hbm)):
        cp = pltpu.make_async_copy(src, xin.at[t], in_sem.at[t])
        cp.start()
        loads.append(cp)
    wload = pltpu.make_async_copy(w_hbm, win, in_sem.at[3])
    wload.start()

    barrier = pltpu.get_barrier_semaphore()
    for d in order:
        pl.semaphore_signal(barrier, inc=1, device_id={"sp": lax.rem(me + d, n)}, device_id_type=MESH)
    for d in range(1, chips):
        pl.semaphore_signal(
            barrier, inc=1, device_id={"dp": lax.rem(chip + d, chips) * 2 + core}, device_id_type=MESH
        )
    pl.semaphore_signal(barrier, inc=1, device_id={"dp": dp + 1 - 2 * core}, device_id_type=MESH)

    lane = lax.broadcasted_iota(jnp.int32, (rows, 128), 1)
    low = lax.rem(lane, 64) < 32
    pos = (lax.broadcasted_iota(jnp.int32, (rows, 128), 0) + me * rows).astype(f32)
    angle = pos * freq_ref[...]
    cos_s[...] = jnp.cos(angle)
    sine = jnp.sin(angle)
    sin_s[...] = jnp.where(low, -sine, sine)

    def widen(t):
        def step(j, _):
            r = pl.ds(pl.multiple_of(j * rows, rows), rows)
            xf[r, :] = xin[t, r, :].astype(f32)
            return 0

        lax.fori_loop(0, n, step, 0)

    def head_rows(h):
        return xf[pl.ds(h, rows, stride=n), :]

    def turned(h):
        x = head_rows(h)
        near = lax.broadcasted_iota(jnp.int32, (rows, 128), 1)
        other = jnp.where(lax.rem(near, 64) < 32, pltpu.roll(x, 96, 1), pltpu.roll(x, 32, 1))
        return x * cos_s[...] + other * sin_s[...]

    def start_all(src, dst, send, recv):
        for d in order:
            peer = lax.rem(me + d, n)
            pltpu.make_async_remote_copy(
                src_ref=src.at[peer],
                dst_ref=dst.at[pl.ds(pl.multiple_of(me * rows, rows), rows)],
                send_sem=send.at[d],
                recv_sem=recv.at[me],
                device_id={"sp": peer},
                device_id_type=MESH,
            ).start()

    mine = pl.ds(pl.multiple_of(me * rows, rows), rows)

    loads[0].wait()
    widen(0)

    def v_step(h, _):
        vs[h] = head_rows(h).astype(bf16)
        return 0

    lax.fori_loop(0, n, v_step, 0)
    loads[1].wait()
    widen(1)

    def k_step(h, _):
        ks[h] = turned(h).astype(bf16)
        return 0

    lax.fori_loop(0, n, k_step, 0)

    pl.semaphore_wait(barrier, n - 1 + chips - 1 + 1)
    start_all(vs, vr, vss, vrs)
    start_all(ks, kr, kss, krs)
    vr[mine, :] = vs[me]
    kr[mine, :] = ks[me]
    loads[2].wait()
    widen(2)

    def q_step(h, _):
        qs[h] = (turned(h) * 0.125).astype(bf16)
        return 0

    lax.fori_loop(0, n, q_step, 0)
    start_all(qs, qr, qss, qrs)
    qr[mine, :] = qs[me]

    wload.wait()
    eye = (
        lax.broadcasted_iota(jnp.int32, (cols, cols), 0) == lax.broadcasted_iota(jnp.int32, (cols, cols), 1)
    ).astype(bf16)

    def w_rows(owner):
        return pl.ds(pl.multiple_of(owner * cols, cols), cols)

    def wt_step(j, _):
        c = pl.ds(pl.multiple_of(j * 256, 256), 256)
        wt[w_rows(dp), c] = dot_nt(eye, win[c, :]).astype(bf16)
        return 0

    lax.fori_loop(0, win.shape[0] // 256, wt_step, 0)
    for d in range(1, chips):
        peer = lax.rem(chip + d, chips) * 2 + core
        pltpu.make_async_remote_copy(
            src_ref=wt.at[w_rows(dp)], dst_ref=wt.at[w_rows(dp)],
            send_sem=wss.at[d], recv_sem=wrs.at[chip],
            device_id={"dp": peer}, device_id_type=MESH,
        ).start()

    for d in order:
        src = lax.rem(me + n - d, n)
        pltpu.make_async_copy(vs.at[0], vr.at[mine], vrs.at[src]).wait()
        pltpu.make_async_copy(vs.at[0], kr.at[mine], krs.at[src]).wait()

    ratio = mix_ref[me]
    ones = jnp.ones((CHUNK, 128), bf16)

    def attend(i):
        q = qr[pl.ds(pl.multiple_of(i * rows, rows), rows), :]
        first = lax.broadcasted_iota(jnp.int32, (rows, 128), 1) < 64
        zero = jnp.zeros_like(q)
        qst[pl.ds(0, rows), :] = jnp.where(first, q, zero)
        qst[pl.ds(rows, rows), :] = jnp.where(first, zero, q)
        mx[...] = jnp.full_like(mx, neg_large)
        acc[...] = jnp.zeros_like(acc)
        count = lax.div((i + 1) * rows + CHUNK - 1, CHUNK)

        def chunk_rows(c):
            return pl.ds(pl.multiple_of(c * CHUNK, CHUNK), CHUNK)

        def put(c, s):
            sc[c] = s
            m = mx[...]
            for b in range(CHUNK // 128):
                m = jnp.maximum(m, s[:, b * 128 : (b + 1) * 128])
            mx[...] = m

        def score_step(c, _):
            put(c, dot_nt(qst[...], kr[chunk_rows(c), :]))
            return 0

        lax.fori_loop(0, count - 1, score_step, 0)
        last = count - 1
        s = dot_nt(qst[...], kr[chunk_rows(last), :])
        row = lax.broadcasted_iota(jnp.int32, (2 * rows, CHUNK), 0)
        row = jnp.where(row >= rows, row - rows, row) + i * rows
        col = lax.broadcasted_iota(jnp.int32, (2 * rows, CHUNK), 1) + last * CHUNK
        put(last, jnp.where(row >= col, s, neg_large))
        highest = jnp.max(mx[...], axis=1, keepdims=True)
        mx[...] = jnp.broadcast_to(highest, mx.shape)

        def weigh_step(c, _):
            m = mx[...]
            p = jnp.exp(sc[c] - jnp.concatenate([m] * (CHUNK // 128), axis=1)).astype(bf16)
            v = jnp.concatenate([vr[chunk_rows(c), :], ones], axis=1)
            acc[...] += jnp.dot(p, v, preferred_element_type=f32)
            return 0

        lax.fori_loop(0, count, weigh_step, 0)
        a = acc[...]
        mixed = a[:rows, :128] / a[:rows, 128:] - ratio * (a[rows:, :128] / a[rows:, 128:])
        scale = lax.rsqrt(jnp.mean(mixed * mixed, axis=1, keepdims=True) + norm_eps)
        return (mixed * scale * gain_ref[...]).astype(bf16)

    ar[me] = attend(me)

    def block_step(t, _):
        d = lax.div(t + 2, 2)
        i = lax.rem(jnp.where(lax.rem(t, 2) == 0, me + n - d, me + d), n)
        rows_i = pl.ds(pl.multiple_of(i * rows, rows), rows)
        pltpu.make_async_copy(vs.at[0], qr.at[rows_i], qrs.at[i]).wait()
        ob[i] = attend(i)
        pltpu.make_async_remote_copy(
            src_ref=ob.at[i], dst_ref=ar.at[me],
            send_sem=oss.at[i], recv_sem=ars.at[me],
            device_id={"sp": i}, device_id_type=MESH,
        ).start()
        return 0

    lax.fori_loop(0, n - 1, block_step, 0)

    partner = dp + 1 - 2 * core
    for d in range(0, chips):
        owner_chip = lax.rem(chip + chips - d, chips)
        owner = owner_chip * 2 + core
        if d:
            pltpu.make_async_copy(wt.at[w_rows(dp)], wt.at[w_rows(owner)], wrs.at[owner_chip]).wait()
        pltpu.make_async_remote_copy(
            src_ref=wt.at[w_rows(owner)], dst_ref=wt.at[w_rows(owner)],
            send_sem=wfs.at[owner_chip], recv_sem=wfr.at[owner_chip],
            device_id={"dp": partner}, device_id_type=MESH,
        ).start()
    for j in range(chips):
        other = j * 2 + 1 - core
        pltpu.make_async_copy(wt.at[w_rows(dp)], wt.at[w_rows(other)], wfr.at[j]).wait()

    def project(h, first):
        part = dot_nt(ar[h], wt[:, pl.ds(pl.multiple_of(h * 128, 128), 128)])
        if first:
            oacc[...] = part
        else:
            oacc[...] += part

    project(me, True)

    def project_step(t, _):
        d = lax.div(t + 2, 2)
        h = lax.rem(jnp.where(lax.rem(t, 2) == 0, me + n - d, me + d), n)
        pltpu.make_async_copy(vs.at[0], ar.at[h], ars.at[h]).wait()
        project(h, False)
        return 0

    lax.fori_loop(0, n - 1, project_step, 0)
    out_ref[...] = oacc[...].astype(bf16)

    for d in order:
        peer = lax.rem(me + d, n)
        pltpu.make_async_copy(vs.at[0], vr.at[mine], vss.at[d]).wait()
        pltpu.make_async_copy(vs.at[0], vr.at[mine], kss.at[d]).wait()
        pltpu.make_async_copy(vs.at[0], vr.at[mine], qss.at[d]).wait()
        pltpu.make_async_copy(vs.at[0], vr.at[mine], oss.at[peer]).wait()
    for d in range(1, chips):
        pltpu.make_async_copy(wt.at[w_rows(dp)], wt.at[w_rows(dp)], wss.at[d]).wait()
    for j in range(chips):
        pltpu.make_async_copy(wt.at[w_rows(dp)], wt.at[w_rows(dp)], wfs.at[j]).wait()


def on_device(queries, keys, values, mix_ratio, out_gain, out_weight):
    n = lax.axis_size("sp")
    cores = lax.axis_size("dp")
    _, rows, heads, width = queries.shape
    depth, cols = out_weight.shape
    total = n * rows
    half = width // 4
    freqs = theta_base ** (-np.arange(half, dtype=np.float32) * np.float32(2.0) / np.float32(width // 2))
    freqs = jnp.asarray(np.tile(freqs.astype(np.float32), 4)[None, :])
    hbm = pl.BlockSpec(memory_space=pltpu.MemorySpace.HBM)
    vmem = pl.BlockSpec(memory_space=pltpu.VMEM)
    dma = pltpu.SemaphoreType.DMA

    def flat(x):
        return x.reshape(rows * heads, width)

    out = pl.pallas_call(
        functools.partial(kernel, n, cores, rows, cols),
        out_shape=jax.ShapeDtypeStruct((rows, cores * cols), bf16),
        in_specs=[pl.BlockSpec(memory_space=pltpu.SMEM), hbm, hbm, hbm, vmem, vmem, hbm],
        out_specs=vmem,
        scratch_shapes=[
            pltpu.VMEM((3, rows * heads, width), bf16),
            pltpu.VMEM((depth, cols), bf16),
            pltpu.VMEM((rows * heads, width), f32),
            pltpu.VMEM((rows, width), f32),
            pltpu.VMEM((rows, width), f32),
            pltpu.VMEM((n, rows, width), bf16),
            pltpu.VMEM((n, rows, width), bf16),
            pltpu.VMEM((n, rows, width), bf16),
            pltpu.VMEM((total, width), bf16),
            pltpu.VMEM((total, width), bf16),
            pltpu.VMEM((total, width), bf16),
            pltpu.VMEM((n, rows, width), bf16),
            pltpu.VMEM((n, rows, width), bf16),
            pltpu.VMEM((cores * cols, depth), bf16),
            pltpu.VMEM((2 * rows, width), bf16),
            pltpu.VMEM((total // CHUNK, 2 * rows, CHUNK), f32),
            pltpu.VMEM((2 * rows, 128), f32),
            pltpu.VMEM((2 * rows, 256), f32),
            pltpu.VMEM((rows, cores * cols), f32),
            dma((4,)),
            dma((n,)), dma((n,)), dma((n,)), dma((n,)), dma((cores // 2,)), dma((cores // 2,)),
            dma((n,)), dma((n,)), dma((n,)), dma((n,)), dma((cores // 2,)), dma((cores // 2,)),
        ],
        compiler_params=pltpu.CompilerParams(
            collective_id=0, has_side_effects=True, vmem_limit_bytes=60 * 2**20
        ),
    )(mix_ratio, flat(queries), flat(keys), flat(values), out_gain.reshape(1, width), freqs, out_weight)
    return out[None]


def solution(mesh):
    tokens = P("dp", "sp", None, None)
    return jax.shard_map(
        on_device,
        mesh=mesh,
        in_specs=(tokens, tokens, tokens, P(), P(), P(None, "dp")),
        out_specs=P("dp", "sp", None),
        check_vma=False,
    )
```

```python
import functools

import jax
import jax.numpy as jnp
import numpy as np
from jax import lax
from jax.experimental import pallas as pl
from jax.experimental.pallas import tpu as pltpu
from jax.sharding import PartitionSpec as P

theta_base = 500000.0
neg_large = -1e30
norm_eps = 1e-05
MESH = pl.DeviceIdType.MESH
f32, bf16 = jnp.float32, jnp.bfloat16
CHUNK = 384


def peer_order(n):
    order = []
    for d in range(1, n // 2 + 1):
        order.append(d)
        if n - d != d:
            order.append(n - d)
    return order


def dot_nt(a, b):
    return lax.dot_general(a, b, (((1,), (1,)), ((), ())), preferred_element_type=f32)


def kernel(
    n, cores, rows, cols,
    mix_ref, q_hbm, k_hbm, v_hbm, gain_ref, freq_ref, w_hbm, out_ref,
    xin, xf, cos_s, sin_s, vs, ks, qs, vr, kr, qr, ob, ar, wt, qst, sc, mx, acc, oacc,
    in_sem, vss, kss, qss, oss, wss, wfs, vrs, krs, qrs, ars, wrs, wfr,
):
    me = lax.axis_index("sp")
    dp = lax.axis_index("dp")
    core = lax.rem(dp, 2)
    chip = lax.div(dp, 2)
    chips = cores // 2
    order = peer_order(n)

    loads = []
    for t, src in enumerate((v_hbm, k_hbm, q_hbm)):
        cp = pltpu.make_async_copy(src, xin.at[t], in_sem.at[t])
        cp.start()
        loads.append(cp)
    own_w = pl.ds(pl.multiple_of(dp * cols, cols), cols)
    wload = pltpu.make_async_copy(w_hbm, wt.at[own_w], in_sem.at[3])
    wload.start()

    barrier = pltpu.get_barrier_semaphore()
    for d in order:
        pl.semaphore_signal(barrier, inc=1, device_id={"sp": lax.rem(me + d, n)}, device_id_type=MESH)
    for d in range(1, chips):
        pl.semaphore_signal(
            barrier, inc=1, device_id={"dp": lax.rem(chip + d, chips) * 2 + core}, device_id_type=MESH
        )
    pl.semaphore_signal(barrier, inc=1, device_id={"dp": dp + 1 - 2 * core}, device_id_type=MESH)

    lane = lax.broadcasted_iota(jnp.int32, (rows, 128), 1)
    low = lax.rem(lane, 64) < 32
    pos = (lax.broadcasted_iota(jnp.int32, (rows, 128), 0) + me * rows).astype(f32)
    angle = pos * freq_ref[...]
    cos_s[...] = jnp.cos(angle)
    sine = jnp.sin(angle)
    sin_s[...] = jnp.where(low, -sine, sine)

    def widen(t):
        def step(j, _):
            r = pl.ds(pl.multiple_of(j * rows, rows), rows)
            xf[r, :] = xin[t, r, :].astype(f32)
            return 0

        lax.fori_loop(0, n, step, 0)

    def head_rows(h):
        return xf[pl.ds(h, rows, stride=n), :]

    def turned(h):
        x = head_rows(h)
        near = lax.broadcasted_iota(jnp.int32, (rows, 128), 1)
        other = jnp.where(lax.rem(near, 64) < 32, pltpu.roll(x, 96, 1), pltpu.roll(x, 32, 1))
        return x * cos_s[...] + other * sin_s[...]

    def start_all(src, dst, send, recv):
        for d in order:
            peer = lax.rem(me + d, n)
            pltpu.make_async_remote_copy(
                src_ref=src.at[peer],
                dst_ref=dst.at[pl.ds(pl.multiple_of(me * rows, rows), rows)],
                send_sem=send.at[d],
                recv_sem=recv.at[me],
                device_id={"sp": peer},
                device_id_type=MESH,
            ).start()

    mine = pl.ds(pl.multiple_of(me * rows, rows), rows)

    loads[0].wait()
    widen(0)

    def v_step(h, _):
        vs[h] = head_rows(h).astype(bf16)
        return 0

    lax.fori_loop(0, n, v_step, 0)
    loads[1].wait()
    widen(1)

    def k_step(h, _):
        ks[h] = turned(h).astype(bf16)
        return 0

    lax.fori_loop(0, n, k_step, 0)

    pl.semaphore_wait(barrier, n - 1 + chips - 1 + 1)
    start_all(vs, vr, vss, vrs)
    start_all(ks, kr, kss, krs)
    vr[mine, :] = vs[me]
    kr[mine, :] = ks[me]
    loads[2].wait()
    widen(2)

    def q_step(h, _):
        qs[h] = (turned(h) * 0.125).astype(bf16)
        return 0

    lax.fori_loop(0, n, q_step, 0)
    start_all(qs, qr, qss, qrs)
    qr[mine, :] = qs[me]

    wload.wait()
    def w_rows(owner):
        return pl.ds(pl.multiple_of(owner * cols, cols), cols)

    for d in range(1, chips):
        peer = lax.rem(chip + d, chips) * 2 + core
        pltpu.make_async_remote_copy(
            src_ref=wt.at[w_rows(dp)], dst_ref=wt.at[w_rows(dp)],
            send_sem=wss.at[d], recv_sem=wrs.at[chip],
            device_id={"dp": peer}, device_id_type=MESH,
        ).start()

    for d in order:
        src = lax.rem(me + n - d, n)
        pltpu.make_async_copy(vs.at[0], vr.at[mine], vrs.at[src]).wait()
        pltpu.make_async_copy(vs.at[0], kr.at[mine], krs.at[src]).wait()

    ratio = mix_ref[me]
    ones = jnp.ones((CHUNK, 128), bf16)

    def attend(i):
        q = qr[pl.ds(pl.multiple_of(i * rows, rows), rows), :]
        first = lax.broadcasted_iota(jnp.int32, (rows, 128), 1) < 64
        zero = jnp.zeros_like(q)
        qst[pl.ds(0, rows), :] = jnp.where(first, q, zero)
        qst[pl.ds(rows, rows), :] = jnp.where(first, zero, q)
        mx[...] = jnp.full_like(mx, neg_large)
        acc[...] = jnp.zeros_like(acc)
        count = lax.div((i + 1) * rows + CHUNK - 1, CHUNK)

        def chunk_rows(c):
            return pl.ds(pl.multiple_of(c * CHUNK, CHUNK), CHUNK)

        def put(c, s):
            sc[c] = s
            m = mx[...]
            for b in range(CHUNK // 128):
                m = jnp.maximum(m, s[:, b * 128 : (b + 1) * 128])
            mx[...] = m

        def score_step(c, _):
            put(c, dot_nt(qst[...], kr[chunk_rows(c), :]))
            return 0

        lax.fori_loop(0, count - 1, score_step, 0)
        last = count - 1
        s = dot_nt(qst[...], kr[chunk_rows(last), :])
        row = lax.broadcasted_iota(jnp.int32, (2 * rows, CHUNK), 0)
        row = jnp.where(row >= rows, row - rows, row) + i * rows
        col = lax.broadcasted_iota(jnp.int32, (2 * rows, CHUNK), 1) + last * CHUNK
        put(last, jnp.where(row >= col, s, neg_large))
        highest = jnp.max(mx[...], axis=1, keepdims=True)
        mx[...] = jnp.broadcast_to(highest, mx.shape)

        def weigh_step(c, _):
            m = mx[...]
            p = jnp.exp(sc[c] - jnp.concatenate([m] * (CHUNK // 128), axis=1)).astype(bf16)
            v = jnp.concatenate([vr[chunk_rows(c), :], ones], axis=1)
            acc[...] += jnp.dot(p, v, preferred_element_type=f32)
            return 0

        lax.fori_loop(0, count, weigh_step, 0)
        a = acc[...]
        mixed = a[:rows, :128] / a[:rows, 128:] - ratio * (a[rows:, :128] / a[rows:, 128:])
        scale = lax.rsqrt(jnp.mean(mixed * mixed, axis=1, keepdims=True) + norm_eps)
        return (mixed * scale * gain_ref[...]).astype(bf16)

    ar[me] = attend(me)

    def block_step(t, _):
        d = lax.div(t + 2, 2)
        i = lax.rem(jnp.where(lax.rem(t, 2) == 0, me + n - d, me + d), n)
        rows_i = pl.ds(pl.multiple_of(i * rows, rows), rows)
        pltpu.make_async_copy(vs.at[0], qr.at[rows_i], qrs.at[i]).wait()
        ob[i] = attend(i)
        pltpu.make_async_remote_copy(
            src_ref=ob.at[i], dst_ref=ar.at[me],
            send_sem=oss.at[i], recv_sem=ars.at[me],
            device_id={"sp": i}, device_id_type=MESH,
        ).start()
        return 0

    lax.fori_loop(0, n - 1, block_step, 0)

    partner = dp + 1 - 2 * core
    for d in range(0, chips):
        owner_chip = lax.rem(chip + chips - d, chips)
        owner = owner_chip * 2 + core
        if d:
            pltpu.make_async_copy(wt.at[w_rows(dp)], wt.at[w_rows(owner)], wrs.at[owner_chip]).wait()
        pltpu.make_async_remote_copy(
            src_ref=wt.at[w_rows(owner)], dst_ref=wt.at[w_rows(owner)],
            send_sem=wfs.at[owner_chip], recv_sem=wfr.at[owner_chip],
            device_id={"dp": partner}, device_id_type=MESH,
        ).start()
    for j in range(chips):
        other = j * 2 + 1 - core
        pltpu.make_async_copy(wt.at[w_rows(dp)], wt.at[w_rows(other)], wfr.at[j]).wait()

    def project(h):
        return dot_nt(ar[h], wt[:, pl.ds(pl.multiple_of(h * 128, 128), 128)])

    def arrived(t):
        d = lax.div(t + 2, 2)
        h = lax.rem(jnp.where(lax.rem(t, 2) == 0, me + n - d, me + d), n)
        pltpu.make_async_copy(vs.at[0], ar.at[h], ars.at[h]).wait()
        return h

    oacc[...] = project(me)

    def project_step(t, _):
        oacc[...] += project(arrived(t))
        return 0

    lax.fori_loop(0, n - 2, project_step, 0)
    out_ref[...] = (oacc[...] + project(arrived(n - 2))).astype(bf16)

    for d in order:
        peer = lax.rem(me + d, n)
        pltpu.make_async_copy(vs.at[0], vr.at[mine], vss.at[d]).wait()
        pltpu.make_async_copy(vs.at[0], vr.at[mine], kss.at[d]).wait()
        pltpu.make_async_copy(vs.at[0], vr.at[mine], qss.at[d]).wait()
        pltpu.make_async_copy(vs.at[0], vr.at[mine], oss.at[peer]).wait()
    for d in range(1, chips):
        pltpu.make_async_copy(wt.at[w_rows(dp)], wt.at[w_rows(dp)], wss.at[d]).wait()
    for j in range(chips):
        pltpu.make_async_copy(wt.at[w_rows(dp)], wt.at[w_rows(dp)], wfs.at[j]).wait()


def on_device(queries, keys, values, mix_ratio, out_gain, out_weight):
    n = lax.axis_size("sp")
    cores = lax.axis_size("dp")
    _, rows, heads, width = queries.shape
    depth, cols = out_weight.shape
    total = n * rows
    half = width // 4
    freqs = theta_base ** (-np.arange(half, dtype=np.float32) * np.float32(2.0) / np.float32(width // 2))
    freqs = jnp.asarray(np.tile(freqs.astype(np.float32), 4)[None, :])
    hbm = pl.BlockSpec(memory_space=pltpu.MemorySpace.HBM)
    vmem = pl.BlockSpec(memory_space=pltpu.VMEM)
    dma = pltpu.SemaphoreType.DMA

    def flat(x):
        return x.reshape(rows * heads, width)

    out = pl.pallas_call(
        functools.partial(kernel, n, cores, rows, cols),
        out_shape=pltpu.VMEM((rows, cores * cols), bf16),
        in_specs=[pl.BlockSpec(memory_space=pltpu.SMEM), hbm, hbm, hbm, vmem, vmem, hbm],
        out_specs=vmem,
        scratch_shapes=[
            pltpu.VMEM((3, rows * heads, width), bf16),
            pltpu.VMEM((rows * heads, width), f32),
            pltpu.VMEM((rows, width), f32),
            pltpu.VMEM((rows, width), f32),
            pltpu.VMEM((n, rows, width), bf16),
            pltpu.VMEM((n, rows, width), bf16),
            pltpu.VMEM((n, rows, width), bf16),
            pltpu.VMEM((total, width), bf16),
            pltpu.VMEM((total, width), bf16),
            pltpu.VMEM((total, width), bf16),
            pltpu.VMEM((n, rows, width), bf16),
            pltpu.VMEM((n, rows, width), bf16),
            pltpu.VMEM((cores * cols, depth), bf16),
            pltpu.VMEM((2 * rows, width), bf16),
            pltpu.VMEM((total // CHUNK, 2 * rows, CHUNK), f32),
            pltpu.VMEM((2 * rows, 128), f32),
            pltpu.VMEM((2 * rows, 256), f32),
            pltpu.VMEM((rows, cores * cols), f32),
            dma((4,)),
            dma((n,)), dma((n,)), dma((n,)), dma((n,)), dma((cores // 2,)), dma((cores // 2,)),
            dma((n,)), dma((n,)), dma((n,)), dma((n,)), dma((cores // 2,)), dma((cores // 2,)),
        ],
        compiler_params=pltpu.CompilerParams(
            collective_id=0, has_side_effects=True, vmem_limit_bytes=60 * 2**20
        ),
    )(mix_ratio, flat(queries), flat(keys), flat(values), out_gain.reshape(1, width), freqs, out_weight.T)
    return out[None]


def solution(mesh):
    tokens = P("dp", "sp", None, None)
    return jax.shard_map(
        on_device,
        mesh=mesh,
        in_specs=(tokens, tokens, tokens, P(), P(), P(None, "dp")),
        out_specs=P("dp", "sp", None),
        check_vma=False,
    )
```

```python
import functools

import jax
import jax.numpy as jnp
import numpy as np
from jax import lax
from jax.experimental import pallas as pl
from jax.experimental.pallas import tpu as pltpu
from jax.sharding import PartitionSpec as P

theta_base = 500000.0
neg_large = -1e30
norm_eps = 1e-05
MESH = pl.DeviceIdType.MESH
f32, bf16 = jnp.float32, jnp.bfloat16
EARLIER = (2, 4, 3, 2)
LOW = len(EARLIER)
CHUNK = 384


def peer_order(n):
    order = []
    for d in range(1, n // 2 + 1):
        order.append(d)
        if n - d != d:
            order.append(n - d)
    return order


def dot_nt(a, b):
    return lax.dot_general(a, b, (((1,), (1,)), ((), ())), preferred_element_type=f32)


def kernel(
    n, cores, rows, cols,
    mix_ref, q_hbm, k_hbm, v_hbm, gain_ref, freq_ref, w_hbm, out_ref,
    xin, xf, cos_s, sin_s, vs, ks, qs, vr, kr, qr, ob, ar, wt, qst, sc, mx, acc, oacc,
    in_sem, vss, kss, qss, oss, wss, wfs, vrs, krs, qrs, ars, wrs, wfr,
):
    me = lax.axis_index("sp")
    dp = lax.axis_index("dp")
    core = lax.rem(dp, 2)
    chip = lax.div(dp, 2)
    chips = cores // 2
    order = peer_order(n)

    loads = []
    for t, src in enumerate((v_hbm, k_hbm, q_hbm)):
        cp = pltpu.make_async_copy(src, xin.at[t], in_sem.at[t])
        cp.start()
        loads.append(cp)
    own_w = pl.ds(pl.multiple_of(dp * cols, cols), cols)
    wload = pltpu.make_async_copy(w_hbm, wt.at[own_w], in_sem.at[3])
    wload.start()

    barrier = pltpu.get_barrier_semaphore()
    for d in order:
        pl.semaphore_signal(barrier, inc=1, device_id={"sp": lax.rem(me + d, n)}, device_id_type=MESH)
    for d in range(1, chips):
        pl.semaphore_signal(
            barrier, inc=1, device_id={"dp": lax.rem(chip + d, chips) * 2 + core}, device_id_type=MESH
        )
    pl.semaphore_signal(barrier, inc=1, device_id={"dp": dp + 1 - 2 * core}, device_id_type=MESH)

    lane = lax.broadcasted_iota(jnp.int32, (rows, 128), 1)
    low = lax.rem(lane, 64) < 32
    pos = (lax.broadcasted_iota(jnp.int32, (rows, 128), 0) + me * rows).astype(f32)
    angle = pos * freq_ref[...]
    cos_s[...] = jnp.cos(angle)
    sine = jnp.sin(angle)
    sin_s[...] = jnp.where(low, -sine, sine)

    def widen(t):
        def step(j, _):
            r = pl.ds(pl.multiple_of(j * rows, rows), rows)
            xf[r, :] = xin[t, r, :].astype(f32)
            return 0

        lax.fori_loop(0, n, step, 0)

    def head_rows(h):
        return xf[pl.ds(h, rows, stride=n), :]

    def turned(h):
        x = head_rows(h)
        near = lax.broadcasted_iota(jnp.int32, (rows, 128), 1)
        other = jnp.where(lax.rem(near, 64) < 32, pltpu.roll(x, 96, 1), pltpu.roll(x, 32, 1))
        return x * cos_s[...] + other * sin_s[...]

    def start_all(src, dst, send, recv):
        for d in order:
            peer = lax.rem(me + d, n)
            pltpu.make_async_remote_copy(
                src_ref=src.at[peer],
                dst_ref=dst.at[pl.ds(pl.multiple_of(me * rows, rows), rows)],
                send_sem=send.at[d],
                recv_sem=recv.at[me],
                device_id={"sp": peer},
                device_id_type=MESH,
            ).start()

    mine = pl.ds(pl.multiple_of(me * rows, rows), rows)

    loads[0].wait()
    widen(0)

    def v_step(h, _):
        vs[h] = head_rows(h).astype(bf16)
        return 0

    lax.fori_loop(0, n, v_step, 0)
    loads[1].wait()
    widen(1)

    def k_step(h, _):
        ks[h] = turned(h).astype(bf16)
        return 0

    lax.fori_loop(0, n, k_step, 0)

    pl.semaphore_wait(barrier, n - 1 + chips - 1 + 1)
    start_all(vs, vr, vss, vrs)
    start_all(ks, kr, kss, krs)
    vr[mine, :] = vs[me]
    kr[mine, :] = ks[me]
    loads[2].wait()
    widen(2)

    def q_step(h, _):
        qs[h] = (turned(h) * 0.125).astype(bf16)
        return 0

    lax.fori_loop(0, n, q_step, 0)
    start_all(qs, qr, qss, qrs)
    qr[mine, :] = qs[me]

    wload.wait()
    def w_rows(owner):
        return pl.ds(pl.multiple_of(owner * cols, cols), cols)

    for d in range(1, chips):
        peer = lax.rem(chip + d, chips) * 2 + core
        pltpu.make_async_remote_copy(
            src_ref=wt.at[w_rows(dp)], dst_ref=wt.at[w_rows(dp)],
            send_sem=wss.at[d], recv_sem=wrs.at[chip],
            device_id={"dp": peer}, device_id_type=MESH,
        ).start()

    for d in order:
        src = lax.rem(me + n - d, n)
        pltpu.make_async_copy(vs.at[0], vr.at[mine], vrs.at[src]).wait()
        pltpu.make_async_copy(vs.at[0], kr.at[mine], krs.at[src]).wait()

    ratio = mix_ref[me]
    ones = jnp.ones((CHUNK, 128), bf16)

    def attend(i):
        q = qr[pl.ds(pl.multiple_of(i * rows, rows), rows), :]
        first = lax.broadcasted_iota(jnp.int32, (rows, 128), 1) < 64
        zero = jnp.zeros_like(q)
        qst[pl.ds(0, rows), :] = jnp.where(first, q, zero)
        qst[pl.ds(rows, rows), :] = jnp.where(first, zero, q)
        mx[...] = jnp.full_like(mx, neg_large)
        acc[...] = jnp.zeros_like(acc)
        count = lax.div((i + 1) * rows + CHUNK - 1, CHUNK)

        def chunk_rows(c):
            return pl.ds(pl.multiple_of(c * CHUNK, CHUNK), CHUNK)

        def put(c, s):
            sc[c] = s
            m = mx[...]
            for b in range(CHUNK // 128):
                m = jnp.maximum(m, s[:, b * 128 : (b + 1) * 128])
            mx[...] = m

        def score_step(c, _):
            put(c, dot_nt(qst[...], kr[chunk_rows(c), :]))
            return 0

        lax.fori_loop(0, count - 1, score_step, 0)
        last = count - 1
        s = dot_nt(qst[...], kr[chunk_rows(last), :])
        row = lax.broadcasted_iota(jnp.int32, (2 * rows, CHUNK), 0)
        row = jnp.where(row >= rows, row - rows, row) + i * rows
        col = lax.broadcasted_iota(jnp.int32, (2 * rows, CHUNK), 1) + last * CHUNK
        put(last, jnp.where(row >= col, s, neg_large))
        highest = jnp.max(mx[...], axis=1, keepdims=True)
        mx[...] = jnp.broadcast_to(highest, mx.shape)

        def weigh_step(c, _):
            m = mx[...]
            p = jnp.exp(sc[c] - jnp.concatenate([m] * (CHUNK // 128), axis=1)).astype(bf16)
            v = jnp.concatenate([vr[chunk_rows(c), :], ones], axis=1)
            acc[...] += jnp.dot(p, v, preferred_element_type=f32)
            return 0

        lax.fori_loop(0, count, weigh_step, 0)
        a = acc[...]
        mixed = a[:rows, :128] / a[:rows, 128:] - ratio * (a[rows:, :128] / a[rows:, 128:])
        scale = lax.rsqrt(jnp.mean(mixed * mixed, axis=1, keepdims=True) + norm_eps)
        return (mixed * scale * gain_ref[...]).astype(bf16)

    ar[me] = attend(me)

    def place(t):
        d = lax.div(t + 2, 2)
        return lax.rem(jnp.where(lax.rem(t, 2) == 0, me + n - d, me + d), n)

    def serve(i):
        rows_i = pl.ds(pl.multiple_of(i * rows, rows), rows)
        pltpu.make_async_copy(vs.at[0], qr.at[rows_i], qrs.at[i]).wait()
        ob[i] = attend(i)
        pltpu.make_async_remote_copy(
            src_ref=ob.at[i], dst_ref=ar.at[me],
            send_sem=oss.at[i], recv_sem=ars.at[me],
            device_id={"sp": i}, device_id_type=MESH,
        ).start()

    def block_step(t, _):
        def early_step(i, _):
            r = lax.rem(me - i + n, n)
            shift = EARLIER[0]
            for q in range(1, LOW):
                shift = jnp.where(i == q, EARLIER[q], shift)
            turn = jnp.maximum(jnp.where(r <= n // 2, 2 * r - 2, 2 * (n - r) - 1) - shift, 0)

            @pl.when((i != me) & (turn == t))
            def _():
                serve(i)

            return 0

        lax.fori_loop(0, LOW, early_step, 0)
        i = place(t)

        @pl.when(i >= LOW)
        def _():
            serve(i)

        return 0

    lax.fori_loop(0, n - 1, block_step, 0)

    partner = dp + 1 - 2 * core
    for d in range(0, chips):
        owner_chip = lax.rem(chip + chips - d, chips)
        owner = owner_chip * 2 + core
        if d:
            pltpu.make_async_copy(wt.at[w_rows(dp)], wt.at[w_rows(owner)], wrs.at[owner_chip]).wait()
        pltpu.make_async_remote_copy(
            src_ref=wt.at[w_rows(owner)], dst_ref=wt.at[w_rows(owner)],
            send_sem=wfs.at[owner_chip], recv_sem=wfr.at[owner_chip],
            device_id={"dp": partner}, device_id_type=MESH,
        ).start()
    for j in range(chips):
        other = j * 2 + 1 - core
        pltpu.make_async_copy(wt.at[w_rows(dp)], wt.at[w_rows(other)], wfr.at[j]).wait()

    def project(h):
        return dot_nt(ar[h], wt[:, pl.ds(pl.multiple_of(h * 128, 128), 128)])

    def arrived(t):
        h = place(t)
        pltpu.make_async_copy(vs.at[0], ar.at[h], ars.at[h]).wait()
        return h

    oacc[...] = project(me)

    def project_step(t, _):
        oacc[...] += project(arrived(t))
        return 0

    lax.fori_loop(0, n - 2, project_step, 0)
    out_ref[...] = (oacc[...] + project(arrived(n - 2))).astype(bf16)

    for d in order:
        peer = lax.rem(me + d, n)
        pltpu.make_async_copy(vs.at[0], vr.at[mine], vss.at[d]).wait()
        pltpu.make_async_copy(vs.at[0], vr.at[mine], kss.at[d]).wait()
        pltpu.make_async_copy(vs.at[0], vr.at[mine], qss.at[d]).wait()
        pltpu.make_async_copy(vs.at[0], vr.at[mine], oss.at[peer]).wait()
    for d in range(1, chips):
        pltpu.make_async_copy(wt.at[w_rows(dp)], wt.at[w_rows(dp)], wss.at[d]).wait()
    for j in range(chips):
        pltpu.make_async_copy(wt.at[w_rows(dp)], wt.at[w_rows(dp)], wfs.at[j]).wait()


def on_device(queries, keys, values, mix_ratio, out_gain, out_weight):
    n = lax.axis_size("sp")
    cores = lax.axis_size("dp")
    _, rows, heads, width = queries.shape
    depth, cols = out_weight.shape
    total = n * rows
    half = width // 4
    freqs = theta_base ** (-np.arange(half, dtype=np.float32) * np.float32(2.0) / np.float32(width // 2))
    freqs = jnp.asarray(np.tile(freqs.astype(np.float32), 4)[None, :])
    hbm = pl.BlockSpec(memory_space=pltpu.MemorySpace.HBM)
    vmem = pl.BlockSpec(memory_space=pltpu.VMEM)
    dma = pltpu.SemaphoreType.DMA

    def flat(x):
        return x.reshape(rows * heads, width)

    out = pl.pallas_call(
        functools.partial(kernel, n, cores, rows, cols),
        out_shape=pltpu.VMEM((rows, cores * cols), bf16),
        in_specs=[pl.BlockSpec(memory_space=pltpu.SMEM), hbm, hbm, hbm, vmem, vmem, hbm],
        out_specs=vmem,
        scratch_shapes=[
            pltpu.VMEM((3, rows * heads, width), bf16),
            pltpu.VMEM((rows * heads, width), f32),
            pltpu.VMEM((rows, width), f32),
            pltpu.VMEM((rows, width), f32),
            pltpu.VMEM((n, rows, width), bf16),
            pltpu.VMEM((n, rows, width), bf16),
            pltpu.VMEM((n, rows, width), bf16),
            pltpu.VMEM((total, width), bf16),
            pltpu.VMEM((total, width), bf16),
            pltpu.VMEM((total, width), bf16),
            pltpu.VMEM((n, rows, width), bf16),
            pltpu.VMEM((n, rows, width), bf16),
            pltpu.VMEM((cores * cols, depth), bf16),
            pltpu.VMEM((2 * rows, width), bf16),
            pltpu.VMEM((total // CHUNK, 2 * rows, CHUNK), f32),
            pltpu.VMEM((2 * rows, 128), f32),
            pltpu.VMEM((2 * rows, 256), f32),
            pltpu.VMEM((rows, cores * cols), f32),
            dma((4,)),
            dma((n,)), dma((n,)), dma((n,)), dma((n,)), dma((cores // 2,)), dma((cores // 2,)),
            dma((n,)), dma((n,)), dma((n,)), dma((n,)), dma((cores // 2,)), dma((cores // 2,)),
        ],
        compiler_params=pltpu.CompilerParams(
            collective_id=0, has_side_effects=True, vmem_limit_bytes=60 * 2**20
        ),
    )(mix_ratio, flat(queries), flat(keys), flat(values), out_gain.reshape(1, width), freqs, out_weight.T)
    return out[None]


def solution(mesh):
    tokens = P("dp", "sp", None, None)
    return jax.shard_map(
        on_device,
        mesh=mesh,
        in_specs=(tokens, tokens, tokens, P(), P(), P(None, "dp")),
        out_specs=P("dp", "sp", None),
        check_vma=False,
    )
```

```python
import functools

import jax
import jax.numpy as jnp
import numpy as np
from jax import lax
from jax.experimental import pallas as pl
from jax.experimental.pallas import tpu as pltpu
from jax.sharding import PartitionSpec as P

theta_base = 500000.0
neg_large = -1e30
norm_eps = 1e-05
MESH = pl.DeviceIdType.MESH
f32, bf16 = jnp.float32, jnp.bfloat16
EARLIER = (2, 4, 2, 2)
LOW = len(EARLIER)
CHUNK = 384


def peer_order(n):
    order = []
    for d in range(1, n // 2 + 1):
        order.append(d)
        if n - d != d:
            order.append(n - d)
    return order


def dot_nt(a, b):
    return lax.dot_general(a, b, (((1,), (1,)), ((), ())), preferred_element_type=f32)


def kernel(
    n, cores, rows, cols,
    mix_ref, q_hbm, k_hbm, v_hbm, gain_ref, freq_ref, w_hbm, out_ref,
    xin, xf, cos_s, sin_s, vs, ks, qs, vr, kr, qr, ob, ar, wt, qst, sc, mx, acc, oacc,
    in_sem, vss, kss, qss, oss, wss, wfs, vrs, krs, qrs, ars, wrs, wfr,
):
    me = lax.axis_index("sp")
    dp = lax.axis_index("dp")
    core = lax.rem(dp, 2)
    chip = lax.div(dp, 2)
    chips = cores // 2
    order = peer_order(n)

    loads = []
    for t, src in enumerate((v_hbm, k_hbm, q_hbm)):
        cp = pltpu.make_async_copy(src, xin.at[t], in_sem.at[t])
        cp.start()
        loads.append(cp)
    own_w = pl.ds(pl.multiple_of(dp * cols, cols), cols)
    wload = pltpu.make_async_copy(w_hbm, wt.at[own_w], in_sem.at[3])
    wload.start()

    barrier = pltpu.get_barrier_semaphore()
    for d in order:
        pl.semaphore_signal(barrier, inc=1, device_id={"sp": lax.rem(me + d, n)}, device_id_type=MESH)
    for d in range(1, chips):
        pl.semaphore_signal(
            barrier, inc=1, device_id={"dp": lax.rem(chip + d, chips) * 2 + core}, device_id_type=MESH
        )
    pl.semaphore_signal(barrier, inc=1, device_id={"dp": dp + 1 - 2 * core}, device_id_type=MESH)

    lane = lax.broadcasted_iota(jnp.int32, (rows, 128), 1)
    low = lax.rem(lane, 64) < 32
    pos = (lax.broadcasted_iota(jnp.int32, (rows, 128), 0) + me * rows).astype(f32)
    angle = pos * freq_ref[...]
    cos_s[...] = jnp.cos(angle)
    sine = jnp.sin(angle)
    sin_s[...] = jnp.where(low, -sine, sine)

    def widen(t):
        def step(j, _):
            r = pl.ds(pl.multiple_of(j * rows, rows), rows)
            xf[r, :] = xin[t, r, :].astype(f32)
            return 0

        lax.fori_loop(0, n, step, 0)

    def head_rows(h):
        return xf[pl.ds(h, rows, stride=n), :]

    def turned(h):
        x = head_rows(h)
        near = lax.broadcasted_iota(jnp.int32, (rows, 128), 1)
        other = jnp.where(lax.rem(near, 64) < 32, pltpu.roll(x, 96, 1), pltpu.roll(x, 32, 1))
        return x * cos_s[...] + other * sin_s[...]

    def start_all(src, dst, send, recv):
        for d in order:
            peer = lax.rem(me + d, n)
            pltpu.make_async_remote_copy(
                src_ref=src.at[peer],
                dst_ref=dst.at[pl.ds(pl.multiple_of(me * rows, rows), rows)],
                send_sem=send.at[d],
                recv_sem=recv.at[me],
                device_id={"sp": peer},
                device_id_type=MESH,
            ).start()

    mine = pl.ds(pl.multiple_of(me * rows, rows), rows)

    loads[0].wait()
    widen(0)

    def v_step(h, _):
        vs[h] = head_rows(h).astype(bf16)
        return 0

    lax.fori_loop(0, n, v_step, 0)
    loads[1].wait()
    widen(1)

    def k_step(h, _):
        ks[h] = turned(h).astype(bf16)
        return 0

    lax.fori_loop(0, n, k_step, 0)

    pl.semaphore_wait(barrier, n - 1 + chips - 1 + 1)
    start_all(vs, vr, vss, vrs)
    start_all(ks, kr, kss, krs)
    vr[mine, :] = vs[me]
    kr[mine, :] = ks[me]
    loads[2].wait()
    widen(2)

    def q_step(h, _):
        qs[h] = (turned(h) * 0.125).astype(bf16)
        return 0

    lax.fori_loop(0, n, q_step, 0)
    start_all(qs, qr, qss, qrs)
    qr[mine, :] = qs[me]

    wload.wait()
    def w_rows(owner):
        return pl.ds(pl.multiple_of(owner * cols, cols), cols)

    for d in range(1, chips):
        peer = lax.rem(chip + d, chips) * 2 + core
        pltpu.make_async_remote_copy(
            src_ref=wt.at[w_rows(dp)], dst_ref=wt.at[w_rows(dp)],
            send_sem=wss.at[d], recv_sem=wrs.at[chip],
            device_id={"dp": peer}, device_id_type=MESH,
        ).start()

    for d in order:
        src = lax.rem(me + n - d, n)
        pltpu.make_async_copy(vs.at[0], vr.at[mine], vrs.at[src]).wait()
        pltpu.make_async_copy(vs.at[0], kr.at[mine], krs.at[src]).wait()

    ratio = mix_ref[me]
    ones = jnp.ones((CHUNK, 128), bf16)

    def attend(i):
        q = qr[pl.ds(pl.multiple_of(i * rows, rows), rows), :]
        first = lax.broadcasted_iota(jnp.int32, (rows, 128), 1) < 64
        zero = jnp.zeros_like(q)
        qst[pl.ds(0, rows), :] = jnp.where(first, q, zero)
        qst[pl.ds(rows, rows), :] = jnp.where(first, zero, q)
        mx[...] = jnp.full_like(mx, neg_large)
        acc[...] = jnp.zeros_like(acc)
        count = lax.div((i + 1) * rows + CHUNK - 1, CHUNK)

        def chunk_rows(c):
            return pl.ds(pl.multiple_of(c * CHUNK, CHUNK), CHUNK)

        def put(c, s):
            sc[c] = s
            m = mx[...]
            for b in range(CHUNK // 128):
                m = jnp.maximum(m, s[:, b * 128 : (b + 1) * 128])
            mx[...] = m

        def score_step(c, _):
            put(c, dot_nt(qst[...], kr[chunk_rows(c), :]))
            return 0

        lax.fori_loop(0, count - 1, score_step, 0)
        last = count - 1
        s = dot_nt(qst[...], kr[chunk_rows(last), :])
        row = lax.broadcasted_iota(jnp.int32, (2 * rows, CHUNK), 0)
        row = jnp.where(row >= rows, row - rows, row) + i * rows
        col = lax.broadcasted_iota(jnp.int32, (2 * rows, CHUNK), 1) + last * CHUNK
        put(last, jnp.where(row >= col, s, neg_large))
        highest = jnp.max(mx[...], axis=1, keepdims=True)
        mx[...] = jnp.broadcast_to(highest, mx.shape)

        def weigh_step(c, _):
            m = mx[...]
            p = jnp.exp(sc[c] - jnp.concatenate([m] * (CHUNK // 128), axis=1)).astype(bf16)
            v = jnp.concatenate([vr[chunk_rows(c), :], ones], axis=1)
            acc[...] += jnp.dot(p, v, preferred_element_type=f32)
            return 0

        lax.fori_loop(0, count, weigh_step, 0)
        a = acc[...]
        mixed = a[:rows, :128] / a[:rows, 128:] - ratio * (a[rows:, :128] / a[rows:, 128:])
        scale = lax.rsqrt(jnp.mean(mixed * mixed, axis=1, keepdims=True) + norm_eps)
        return (mixed * scale * gain_ref[...]).astype(bf16)

    ar[me] = attend(me)

    def place(t):
        d = lax.div(t + 2, 2)
        return lax.rem(jnp.where(lax.rem(t, 2) == 0, me + n - d, me + d), n)

    def serve(i):
        rows_i = pl.ds(pl.multiple_of(i * rows, rows), rows)
        pltpu.make_async_copy(vs.at[0], qr.at[rows_i], qrs.at[i]).wait()
        ob[i] = attend(i)
        pltpu.make_async_remote_copy(
            src_ref=ob.at[i], dst_ref=ar.at[me],
            send_sem=oss.at[i], recv_sem=ars.at[me],
            device_id={"sp": i}, device_id_type=MESH,
        ).start()

    def block_step(t, _):
        def early_step(i, _):
            r = lax.rem(me - i + n, n)
            shift = EARLIER[0]
            for q in range(1, LOW):
                shift = jnp.where(i == q, EARLIER[q], shift)
            turn = jnp.maximum(jnp.where(r <= n // 2, 2 * r - 2, 2 * (n - r) - 1) - shift, 0)

            @pl.when((i != me) & (turn == t))
            def _():
                serve(i)

            return 0

        lax.fori_loop(0, LOW, early_step, 0)
        i = place(t)

        @pl.when(i >= LOW)
        def _():
            serve(i)

        return 0

    lax.fori_loop(0, n - 1, block_step, 0)

    partner = dp + 1 - 2 * core
    for d in range(0, chips):
        owner_chip = lax.rem(chip + chips - d, chips)
        owner = owner_chip * 2 + core
        if d:
            pltpu.make_async_copy(wt.at[w_rows(dp)], wt.at[w_rows(owner)], wrs.at[owner_chip]).wait()
        pltpu.make_async_remote_copy(
            src_ref=wt.at[w_rows(owner)], dst_ref=wt.at[w_rows(owner)],
            send_sem=wfs.at[owner_chip], recv_sem=wfr.at[owner_chip],
            device_id={"dp": partner}, device_id_type=MESH,
        ).start()
    for j in range(chips):
        other = j * 2 + 1 - core
        pltpu.make_async_copy(wt.at[w_rows(dp)], wt.at[w_rows(other)], wfr.at[j]).wait()

    def project(h):
        return dot_nt(ar[h], wt[:, pl.ds(pl.multiple_of(h * 128, 128), 128)])

    def arrived(t):
        h = place(t)
        pltpu.make_async_copy(vs.at[0], ar.at[h], ars.at[h]).wait()
        return h

    oacc[...] = project(me)

    def project_step(t, _):
        oacc[...] += project(arrived(t))
        return 0

    lax.fori_loop(0, n - 2, project_step, 0)
    out_ref[...] = (oacc[...] + project(arrived(n - 2))).astype(bf16)

    for d in order:
        peer = lax.rem(me + d, n)
        pltpu.make_async_copy(vs.at[0], vr.at[mine], vss.at[d]).wait()
        pltpu.make_async_copy(vs.at[0], vr.at[mine], kss.at[d]).wait()
        pltpu.make_async_copy(vs.at[0], vr.at[mine], qss.at[d]).wait()
        pltpu.make_async_copy(vs.at[0], vr.at[mine], oss.at[peer]).wait()
    for d in range(1, chips):
        pltpu.make_async_copy(wt.at[w_rows(dp)], wt.at[w_rows(dp)], wss.at[d]).wait()
    for j in range(chips):
        pltpu.make_async_copy(wt.at[w_rows(dp)], wt.at[w_rows(dp)], wfs.at[j]).wait()


def on_device(queries, keys, values, mix_ratio, out_gain, out_weight):
    n = lax.axis_size("sp")
    cores = lax.axis_size("dp")
    _, rows, heads, width = queries.shape
    depth, cols = out_weight.shape
    total = n * rows
    half = width // 4
    freqs = theta_base ** (-np.arange(half, dtype=np.float32) * np.float32(2.0) / np.float32(width // 2))
    freqs = jnp.asarray(np.tile(freqs.astype(np.float32), 4)[None, :])
    hbm = pl.BlockSpec(memory_space=pltpu.MemorySpace.HBM)
    vmem = pl.BlockSpec(memory_space=pltpu.VMEM)
    dma = pltpu.SemaphoreType.DMA

    def flat(x):
        return x.reshape(rows * heads, width)

    out = pl.pallas_call(
        functools.partial(kernel, n, cores, rows, cols),
        out_shape=pltpu.VMEM((rows, cores * cols), bf16),
        in_specs=[pl.BlockSpec(memory_space=pltpu.SMEM), hbm, hbm, hbm, vmem, vmem, hbm],
        out_specs=vmem,
        scratch_shapes=[
            pltpu.VMEM((3, rows * heads, width), bf16),
            pltpu.VMEM((rows * heads, width), f32),
            pltpu.VMEM((rows, width), f32),
            pltpu.VMEM((rows, width), f32),
            pltpu.VMEM((n, rows, width), bf16),
            pltpu.VMEM((n, rows, width), bf16),
            pltpu.VMEM((n, rows, width), bf16),
            pltpu.VMEM((total, width), bf16),
            pltpu.VMEM((total, width), bf16),
            pltpu.VMEM((total, width), bf16),
            pltpu.VMEM((n, rows, width), bf16),
            pltpu.VMEM((n, rows, width), bf16),
            pltpu.VMEM((cores * cols, depth), bf16),
            pltpu.VMEM((2 * rows, width), bf16),
            pltpu.VMEM((total // CHUNK, 2 * rows, CHUNK), f32),
            pltpu.VMEM((2 * rows, 128), f32),
            pltpu.VMEM((2 * rows, 256), f32),
            pltpu.VMEM((rows, cores * cols), f32),
            dma((4,)),
            dma((n,)), dma((n,)), dma((n,)), dma((n,)), dma((cores // 2,)), dma((cores // 2,)),
            dma((n,)), dma((n,)), dma((n,)), dma((n,)), dma((cores // 2,)), dma((cores // 2,)),
        ],
        compiler_params=pltpu.CompilerParams(
            collective_id=0, has_side_effects=True, vmem_limit_bytes=60 * 2**20
        ),
    )(mix_ratio, flat(queries), flat(keys), flat(values), out_gain.reshape(1, width), freqs, out_weight.T)
    return out[None]


def solution(mesh):
    tokens = P("dp", "sp", None, None)
    return jax.shard_map(
        on_device,
        mesh=mesh,
        in_specs=(tokens, tokens, tokens, P(), P(), P(None, "dp")),
        out_specs=P("dp", "sp", None),
        check_vma=False,
    )
```
